32 devices in a mesh: ep: 8 (over z, y), tp: 4 (over x, core).
Axes of the slice: x: 2, y: 2, z: 4, core: 2. Of those that a mesh axis runs over, the one named last changes fastest.
Arguments:
- mixer_in: bfloat16 [4096, 4096], P(('ep', 'tp')), may hold values from -6 to 6
- mixer_gain: float32 [4096], replicated, may hold values from 0.1 to 1.9
- group_weight: bfloat16 [4, 1024, 1024], P('tp'), may hold values from -0.1875 to 0.1875
- group_scale: float32 [4, 1024], P('tp'), may hold values from 0.1 to 1.9
- expert_in: bfloat16 [4096, 4096], P(('ep', 'tp')), may hold values from -6 to 6
- expert_gain: float32 [4096], replicated, may hold values from 0.1 to 1.9
- routes: int32 [4096, 2], P('ep'), may hold values from 0 to 7, all different within a row; in each aligned block of 128 rows (0 to 127, 128 to 255, ...) at most 48 rows name the same one
- route_weight: float32 [4096, 2], P('ep'), may hold values from 0.2 to 1
- gate_weight: bfloat16 [8, 4096, 1024], P('ep', None, 'tp'), may hold values from -0.25 to 0.25
- up_weight: bfloat16 [8, 4096, 1024], P('ep', None, 'tp'), may hold values from -0.25 to 0.25
- down_weight: bfloat16 [8, 1024, 4096], P('ep', 'tp'), may hold values from -0.02734375 to 0.02734375
Outputs:
- mixed: bfloat16 [4096, 4096], P('ep', 'tp')
- expert_out: bfloat16 [4096, 4096], P(('ep', 'tp'))
The draws below stay inside these ranges and needn't reach their ends.
Inputs may be any that keep to these rules, and one draw needn't show every extreme that they name: `routes`: each row names 2 different experts; within the rows of one device (aligned blocks of 128 rows) no expert is named more than 48 times, and that count is reached.
All inputs are finite; a program needn't handle non-finite values.
Results may differ from the reference program's by a relative error of at most 0.012.
Values may be sent and summed in bfloat16 or wider, within the bound.
No kernel may reach another device: no remote copies, remote signals or barrier semaphores. Data moves between devices by JAX's collectives and lax.ppermute only.
A program may use at most 128 MiB of HBM per device.

```python
import math
import jax
import jax.numpy as jnp
import numpy as np
from jax import lax

D = 4096
GROUPS = 4
GW = 1024
WMAX = 16
F = 1024
TOP = 2
TOK_B = 128
EXPERTS = 8
CAP = 48
TOKENS_A = 4096
TOKENS_B = 4096
N_TP = 4


def levels(rng, dims, cuts, low, high):
    loudness, own = 1.0, jax.random.fold_in(rng, 6)
    for axis_at, blocks in cuts:
        steps = jnp.exp(jax.random.uniform(jax.random.fold_in(own, axis_at), (blocks,), jnp.float32, low / len(cuts), high / len(cuts)))
        loudness = loudness * jnp.repeat(steps, dims[axis_at] // blocks).reshape([-1 if axis == axis_at else 1 for axis in range(len(dims))])
    return loudness


def assign_block(rng, own, number, rows, amount, top, bound, slope):
    ranking = jax.random.permutation(rng, amount)
    packed, ordinary = portions_of(amount, rows * top, bound, slope, True), portions_of(amount, rows * top, bound, slope, False)
    places = jnp.arange(amount)

    def named(tallies, offset_by):
        used = int((tallies > 0).sum())
        fixed = max(1, used // 4)
        shifted = fixed + (places - fixed + offset_by * (used - fixed)) % max(1, amount - fixed)
        return jnp.zeros((amount,), jnp.int32).at[ranking[jnp.where(places < fixed, places, shifted)]].set(jnp.asarray(tallies, jnp.int32))

    tallies = jnp.where(number % 4 == 0, named(packed, number // 4), named(ordinary, number - number // 4 - 1))
    mixed = jax.random.permutation(jax.random.fold_in(own, 3), amount)
    source_of, receiver = mixed[0:amount // 2 * 2:2], mixed[1:amount // 2 * 2:2]
    slack = jnp.minimum(tallies[source_of] - 1, bound - tallies[receiver]) // 2
    slack = jnp.where((source_of == ranking[0]) | (receiver == ranking[0]) | (tallies[receiver] == 0), 0, jnp.maximum(slack, 0))
    shifted = jax.random.randint(jax.random.fold_in(own, 4), (amount // 2,), 0, 1 << 20) % (slack + 1)
    tallies = tallies.at[source_of].add(-shifted).at[receiver].add(shifted)
    members = jnp.searchsorted(jnp.cumsum(tallies), jnp.arange(rows * top), side="right").astype(jnp.int32)
    listing = members.reshape(top, rows).T
    listing = listing[jax.random.permutation(jax.random.fold_in(own, 1), rows)]
    offset_by = jax.random.randint(jax.random.fold_in(own, 2), (rows, 1), 0, top)
    return jnp.take_along_axis(listing, (jnp.arange(top)[None, :] + offset_by) % top, axis=1)


def portions_of(amount, total, bound, skew, full):
    portions = [(1 << 20) // math.isqrt(rank ** skew) + 1 for rank in range(1, amount + 1)]
    largest = bound if full else min(bound, max(-(-total // amount), total * portions[0] // sum(portions)))
    least = 1 if total - largest >= amount - 1 else 0
    given, surplus = [largest] + [least] * (amount - 1), total - largest - least * (amount - 1)
    while surplus > 0:
        movable = [i for i in range(1, amount) if given[i] < largest] or [i for i in range(1, amount) if given[i] < bound]
        mass, budget = sum([portions[i] for i in movable]), surplus
        for i in movable:
            more = min(bound - given[i], max(1, budget * portions[i] // mass), surplus)
            given[i] = given[i] + more
            surplus = surplus - more
    return np.array(given)


def bell_draw(own_key, extent, width, bound, cuts=(), kind=jnp.bfloat16):
    result = width * jax.random.normal(own_key, extent, jnp.float32)
    if cuts:
        result = result * levels(own_key, extent, cuts, -0.22, 0.18)
    return jnp.clip(result, -bound, bound).astype(kind)


def setup_inputs(seed: int = 0) -> dict:
    key_of = jax.random.split(jax.random.key(seed), 12)
    mixer_in = bell_draw(key_of[0], (TOKENS_A, D), 1.0, 6.0, ((0, 32),))
    mixer_gain = jnp.clip(1.0 + 0.18 * jax.random.normal(key_of[1], (D,), jnp.float32), 0.1, 1.9)
    group_weight = bell_draw(key_of[2], (GROUPS, GW, GW), GW ** -0.5, 0.1875, ((0, 4),))
    group_scale = jnp.clip(1.0 + 0.18 * jax.random.normal(key_of[3], (GROUPS, GW), jnp.float32), 0.1, 1.9)
    expert_in = bell_draw(key_of[4], (TOKENS_B, D), 1.0, 6.0, ((0, 32),))
    expert_gain = jnp.clip(1.0 + 0.18 * jax.random.normal(key_of[5], (D,), jnp.float32), 0.1, 1.9)
    routes_keys = jax.random.split(jax.random.fold_in(key_of[6], 1), TOKENS_B // TOK_B)
    routes_turns = jax.random.permutation(jax.random.fold_in(key_of[6], 3), TOKENS_B // TOK_B)
    routes = jax.vmap(lambda own, number: assign_block(jax.random.fold_in(key_of[6], 2), own, number, TOK_B, EXPERTS, TOP, CAP, 2))(routes_keys, routes_turns).reshape((TOKENS_B, TOP))
    route_weight = jnp.clip(0.2 + 0.8 * jax.random.uniform(key_of[7], (TOKENS_B, TOP), jnp.float32) ** levels(key_of[7], (TOKENS_B, TOP), ((0, 8),), -0.2, 0.2), 0.2, 1.0)
    gate_weight = bell_draw(key_of[8], (EXPERTS, D, F), (D // 9) ** -0.5, 0.25, ((0, 8), (2, 4)))
    up_weight = bell_draw(key_of[9], (EXPERTS, D, F), (D // 9) ** -0.5, 0.25, ((0, 8), (2, 4)))
    down_weight = bell_draw(key_of[10], (EXPERTS, F, D), (45 * F) ** -0.5, 0.02734375, ((0, 8), (1, 4)))
    return {"mixer_in": mixer_in, "mixer_gain": mixer_gain, "group_weight": group_weight, "group_scale": group_scale, "expert_in": expert_in, "expert_gain": expert_gain, "routes": routes, "route_weight": route_weight, "gate_weight": gate_weight, "up_weight": up_weight, "down_weight": down_weight}


epsilon = 1e-06
clamp_limit = 7.0
sigmoid_slope = 1.702

def rms_norm(values, gain):
    widened = values.astype(jnp.float32)
    scaled = widened * lax.rsqrt(lax.optimization_barrier(jnp.mean(widened * widened, axis=-1, keepdims=True)) + epsilon)
    return (scaled * gain).astype(jnp.bfloat16)

def clamped_unit(gate_part, up_part):
    gate_part = jnp.minimum(gate_part, clamp_limit)
    up_part = jnp.clip(up_part, -clamp_limit, clamp_limit)
    return ((up_part + 1.0) * gate_part * jax.nn.sigmoid(sigmoid_slope * gate_part)).astype(jnp.bfloat16)

def slot_table(block_routes, experts, capacity):
    count = block_routes.shape[0]
    onehot = (block_routes[:, :, None] == jnp.arange(experts, dtype=jnp.int32)[None, None, :]).astype(jnp.int32)
    per_token = lax.optimization_barrier(jnp.sum(onehot, axis=1))
    earlier = jnp.cumsum(per_token, axis=0) - per_token
    slot_rank = lax.optimization_barrier(jnp.sum(onehot * earlier[:, None, :], axis=2))
    matches = onehot[:, :, :, None] * (slot_rank[:, :, None, None] == jnp.arange(capacity, dtype=jnp.int32)[None, None, None, :]).astype(jnp.int32)
    source = lax.optimization_barrier(jnp.sum(matches * jnp.arange(count, dtype=jnp.int32)[:, None, None, None], axis=(0, 1)))
    filled = lax.optimization_barrier(jnp.sum(matches, axis=(0, 1)))
    return (source, filled, slot_rank)

def reference(mixer_in, mixer_gain, group_weight, group_scale, expert_in, expert_gain, routes, route_weight, gate_weight, up_weight, down_weight):
    normed = rms_norm(mixer_in, mixer_gain)
    length = normed.shape[0]
    position = jnp.arange(length, dtype=jnp.int32)
    pieces = []
    for group in range(GROUPS):
        window = 2 ** (group + 1)
        values = normed[:, group * GW:(group + 1) * GW].astype(jnp.float32)
        padded = jnp.pad(values, ((WMAX - 1, 0), (0, 0)))
        window_sum = jnp.zeros_like(values)
        for offset in range(window):
            window_sum = window_sum + padded[WMAX - 1 - offset:WMAX - 1 - offset + length]
        counts = jnp.minimum(position + 1, window).astype(jnp.float32)[:, None]
        pooled = (window_sum / counts - values).astype(jnp.bfloat16)
        product = jnp.dot(pooled, group_weight[group], preferred_element_type=jnp.float32)
        pieces.append((product * group_scale[group]).astype(jnp.bfloat16))
    mixed = jnp.concatenate(pieces, axis=1)
    expert_norm = rms_norm(expert_in, expert_gain)
    blocks = expert_norm.shape[0] // TOK_B
    block_routes = routes.reshape(blocks, TOK_B, TOP)
    source, filled, slot_rank = lax.map(lambda item: slot_table(item, EXPERTS, CAP), block_routes)
    global_index = source + (jnp.arange(blocks, dtype=jnp.int32) * TOK_B)[:, None, None]
    part_width = F // N_TP

    def one_expert(expert):
        slot_index = lax.dynamic_index_in_dim(global_index, expert, 1, keepdims=False).reshape(-1)
        present = lax.dynamic_index_in_dim(filled, expert, 1, keepdims=False).reshape(-1)
        picked = expert_norm[slot_index] * present[:, None].astype(jnp.bfloat16)
        gate_part = jnp.dot(picked, gate_weight[expert], preferred_element_type=jnp.float32)
        up_part = jnp.dot(picked, up_weight[expert], preferred_element_type=jnp.float32)
        hidden = clamped_unit(gate_part, up_part)
        total = jnp.zeros((picked.shape[0], picked.shape[1]), jnp.float32)
        for part in range(N_TP):
            partial_value = jnp.dot(hidden[:, part * part_width:(part + 1) * part_width], down_weight[expert][part * part_width:(part + 1) * part_width], preferred_element_type=jnp.float32).astype(jnp.bfloat16)
            total = total + lax.optimization_barrier(partial_value).astype(jnp.float32)
        return total.astype(jnp.bfloat16).reshape(blocks, CAP, picked.shape[1])
    results = lax.map(one_expert, jnp.arange(EXPERTS, dtype=jnp.int32))
    flat_rows = results.reshape(-1, results.shape[-1])
    block_of = (jnp.arange(expert_norm.shape[0], dtype=jnp.int32) // TOK_B)[:, None]
    slot_index = (routes * blocks + block_of) * CAP + slot_rank.reshape(-1, TOP)
    expert_sum = jnp.zeros(expert_norm.shape, jnp.float32)
    for choice_slot in range(TOP):
        expert_sum = expert_sum + flat_rows[slot_index[:, choice_slot]].astype(jnp.float32) * route_weight[:, choice_slot:choice_slot + 1]
    return (mixed, expert_sum.astype(jnp.bfloat16))
```

```python
import functools

import jax
import jax.numpy as jnp
from jax import lax
from jax.experimental import pallas as pl
from jax.experimental.pallas import tpu as pltpu
from jax.sharding import PartitionSpec as P

WMAX = 16
TOP = 2
epsilon = 1e-06
clamp_limit = 7.0
sigmoid_slope = 1.702


F32 = jnp.float32
BF16 = jnp.bfloat16


def swap(x, axis, mask):
    if mask == 0:
        return x
    return lax.ppermute(x, axis, [(i, i ^ mask) for i in range(lax.axis_size(axis))])


def normed_rows(x, gain):
    wide = x.astype(F32)
    mean = jnp.mean(wide * wide, axis=-1, keepdims=True)
    return (wide * lax.rsqrt(mean + epsilon) * gain).astype(BF16)


def split_bf16(x):
    high = x.astype(BF16)
    return high, (x - high.astype(F32)).astype(BF16)


def over_rows(a, b):
    return lax.dot_general(a, b, (((0,), (0,)), ((), ())), preferred_element_type=F32)


def front_body(place, rows, gain, routes, weights, *outs, chunks, slots):
    out_rows, high_out, low_out = outs[:chunks], outs[chunks], outs[chunks + 1]
    count = rows.shape[0]
    normed = normed_rows(rows[...], gain[...])
    distance = routes[...] ^ place[0]
    lane = lax.broadcasted_iota(jnp.int32, (count, chunks), 1)
    onehot = jnp.zeros((count, chunks), F32)
    share = jnp.zeros((count, chunks), F32)
    for choice in range(TOP):
        hit = distance[:, choice : choice + 1] == lane
        onehot = onehot + jnp.where(hit, 1.0, 0.0)
        share = share + jnp.where(hit, weights[:, choice : choice + 1], 0.0)
    first = lax.broadcasted_iota(jnp.int32, (count, count), 0)
    second = lax.broadcasted_iota(jnp.int32, (count, count), 1)
    same = jnp.where(first == second, 1.0, 0.0).astype(BF16)
    before = jnp.where(first < second, 1.0, 0.0).astype(BF16)
    onehot = onehot.astype(BF16)
    present = over_rows(onehot, same)
    rank = over_rows(onehot, before)
    share_high, share_low = split_bf16(share)
    share_high = over_rows(share_high, same)
    share_low = over_rows(share_low, same)
    slot = lax.broadcasted_iota(jnp.int32, (slots, count), 0).astype(F32)
    for k in range(chunks):
        pick = jnp.where(rank[k : k + 1] == slot, present[k : k + 1], 0.0)
        high_out[k * slots : (k + 1) * slots] = (pick * share_high[k : k + 1]).astype(BF16)
        low_out[k * slots : (k + 1) * slots] = (pick * share_low[k : k + 1]).astype(BF16)
        out_rows[k][...] = jnp.dot(pick.astype(BF16), normed, preferred_element_type=F32).astype(BF16)


def front(place, rows, gain, routes, weights, chunks, slots):
    count, width = rows.shape
    whole = lambda shape: pl.BlockSpec(shape, lambda i, s: (0, 0))
    shapes = [jax.ShapeDtypeStruct((slots, width), BF16)] * chunks
    shapes += [jax.ShapeDtypeStruct((chunks * slots, count), BF16)] * 2
    return pl.pallas_call(
        functools.partial(front_body, chunks=chunks, slots=slots),
        out_shape=shapes,
        grid_spec=pltpu.PrefetchScalarGridSpec(
            num_scalar_prefetch=1,
            grid=(1,),
            in_specs=[
                whole((count, width)),
                whole((1, width)),
                pl.BlockSpec((count, TOP), lambda i, s: (s[1], 0)),
                pl.BlockSpec((count, TOP), lambda i, s: (s[1], 0)),
            ],
            out_specs=[whole(s.shape) for s in shapes],
        ),
        name="front",
    )(place, rows, gain, routes, weights)


def hidden_body(*refs, inputs, per_peer, halves, steps):
    rows = refs[:inputs]
    gates = refs[inputs : inputs + halves]
    ups = refs[inputs + halves : inputs + 2 * halves]
    outs = refs[inputs + 2 * halves : -2]
    gate_acc, up_acc = refs[-2:]
    step = pl.program_id(0)
    block = jnp.concatenate([r[...] for r in rows], axis=0)
    part = gates[0].shape[1]
    for acc, weights in ((gate_acc, gates), (up_acc, ups)):
        for h in range(halves):
            product = jnp.dot(block, weights[h][...], preferred_element_type=F32)
            cols = slice(h * part, (h + 1) * part)
            acc[:, cols] = jnp.where(step == 0, product, acc[:, cols] + product)

    @pl.when(step == steps - 1)
    def _():
        gate = jnp.minimum(gate_acc[...], clamp_limit)
        up = jnp.clip(up_acc[...], -clamp_limit, clamp_limit)
        hidden = ((up + 1.0) * gate * jax.nn.sigmoid(sigmoid_slope * gate)).astype(BF16)
        for p, out in enumerate(outs):
            out[...] = hidden[p * per_peer : (p + 1) * per_peer]


def hidden_of(rows_by_peer, gates, ups):
    rows = [r for peer in rows_by_peer for r in peer]
    width = rows[0].shape[1]
    per_peer = sum(r.shape[0] for r in rows_by_peer[0])
    total = per_peer * len(rows_by_peer)
    part = gates[0].shape[1]
    steps = 4
    block = width // steps
    halves = len(gates)
    return pl.pallas_call(
        functools.partial(
            hidden_body, inputs=len(rows), per_peer=per_peer, halves=halves, steps=steps
        ),
        out_shape=[jax.ShapeDtypeStruct((per_peer, part * halves), BF16)] * len(rows_by_peer),
        grid=(steps,),
        in_specs=[pl.BlockSpec((r.shape[0], block), lambda i: (0, i)) for r in rows]
        + [pl.BlockSpec((block, part), lambda i: (i, 0))] * (2 * halves),
        out_specs=[pl.BlockSpec((per_peer, part * halves), lambda i: (0, 0))] * len(rows_by_peer),
        scratch_shapes=[pltpu.VMEM((total, part * halves), F32)] * 2,
        name="hidden",
    )(*rows, *gates, *ups)


def down_body(*refs, peers, parts, outs_count):
    hidden = refs[:peers]
    weights = refs[peers : peers + peers * parts]
    outs = refs[peers + peers * parts :]
    part = weights[0].shape[0]
    total = None
    for p in range(peers):
        for h in range(parts):
            product = jnp.dot(
                hidden[p][:, h * part : (h + 1) * part],
                weights[p * parts + h][...],
                preferred_element_type=F32,
            )
            total = product if total is None else total + product
    total = total.astype(BF16)
    slots = outs[0].shape[0]
    for c in range(outs_count):
        outs[c][...] = total[c * slots : (c + 1) * slots]


def result_of(hidden, weights, chunks, slots):
    peers = len(hidden)
    parts = len(weights) // peers
    part, width = weights[0].shape
    steps = 4
    block = width // steps
    return pl.pallas_call(
        functools.partial(down_body, peers=peers, parts=parts, outs_count=chunks),
        out_shape=[jax.ShapeDtypeStruct((slots, width), BF16)] * chunks,
        grid=(steps,),
        in_specs=[pl.BlockSpec(h.shape, lambda i: (0, 0)) for h in hidden]
        + [pl.BlockSpec((part, block), lambda i: (0, i))] * len(weights),
        out_specs=[pl.BlockSpec((slots, block), lambda i: (0, i))] * chunks,
        name="down",
    )(*hidden, *weights)


def combine_body(high, low, *refs):
    rows = jnp.concatenate([r[...] for r in refs[:-1]], axis=0)
    refs[-1][...] = (over_rows(high[...], rows) + over_rows(low[...], rows)).astype(BF16)


def combine(high, low, chunks):
    slots, width = chunks[0].shape
    count = high.shape[1]
    steps = 4
    block = width // steps
    return pl.pallas_call(
        combine_body,
        out_shape=jax.ShapeDtypeStruct((count, width), BF16),
        grid=(steps,),
        in_specs=[pl.BlockSpec(high.shape, lambda i: (0, 0))] * 2
        + [pl.BlockSpec((slots, block), lambda i: (0, i))] * len(chunks),
        out_specs=pl.BlockSpec((count, block), lambda i: (0, i)),
        name="combine",
    )(high, low, *chunks)


def pool_body(place, halo, rows, gain, *outs, groups):
    count, width = rows.shape
    cols = width // groups
    reach = halo.shape[0]
    square = lambda x: jnp.sum(x.astype(F32) * x.astype(F32), axis=-1, keepdims=True)
    squares = jnp.concatenate([square(halo[...]), square(rows[...])], axis=0)
    scale = lax.rsqrt(squares / width + epsilon)
    position = place[2] + lax.broadcasted_iota(jnp.int32, (count, 1), 0)
    for m in range(groups):
        group = place[1] ^ m
        at = pl.ds(pl.multiple_of(group * cols, cols), cols)
        raw = jnp.concatenate([halo[:, at], rows[:, at]], axis=0).astype(F32)
        values = (raw * scale * gain[:, at]).astype(BF16).astype(F32)
        total = values + pltpu.roll(values, 1, 0)
        chosen = total
        for step in range(1, groups):
            total = total + pltpu.roll(total, 1 << step, 0)
            chosen = jnp.where(group >= step, total, chosen)
        window = jnp.left_shift(2, group)
        counts = jnp.minimum(position + 1, window).astype(F32)
        outs[m][...] = (chosen[reach:] / counts - values[reach:]).astype(BF16)


def pool(place, halo, rows, gain, groups):
    count, width = rows.shape
    whole = lambda shape: pl.BlockSpec(shape, lambda i, s: (0, 0))
    shapes = [jax.ShapeDtypeStruct((count, width // groups), BF16)] * groups
    return pl.pallas_call(
        functools.partial(pool_body, groups=groups),
        out_shape=shapes,
        grid_spec=pltpu.PrefetchScalarGridSpec(
            num_scalar_prefetch=1,
            grid=(1,),
            in_specs=[whole(halo.shape), whole(rows.shape), whole(gain.shape)],
            out_specs=[whole(s.shape) for s in shapes],
        ),
        name="pool",
    )(place, halo, rows, gain)


def mix_body(place, *refs, groups):
    parts, weight, scale, out = refs[:groups], refs[groups], refs[groups + 1], refs[groups + 2]
    count = parts[0].shape[0]
    for m in range(groups):
        product = jnp.dot(parts[m][...], weight[0], preferred_element_type=F32) * scale[...]
        at = pl.multiple_of((place[1] ^ m) * count, count)
        out[pl.ds(at, count)] = product.astype(BF16)


def mix(place, parts, weight, scale):
    groups = len(parts)
    count, cols = parts[0].shape
    whole = lambda shape: pl.BlockSpec(shape, lambda i, s: (0,) * len(shape))
    shape = jax.ShapeDtypeStruct((groups * count, cols), BF16)
    return pl.pallas_call(
        functools.partial(mix_body, groups=groups),
        out_shape=shape,
        grid_spec=pltpu.PrefetchScalarGridSpec(
            num_scalar_prefetch=1,
            grid=(1,),
            in_specs=[whole(p.shape) for p in parts] + [whole(weight.shape), whole(scale.shape)],
            out_specs=whole(shape.shape),
        ),
        name="mix",
    )(place, *parts, weight, scale)


def chunk_groups(experts):
    size = max(1, experts // 4)
    order = list(range(experts // 2, experts)) + list(range(experts // 2))
    return [order[at : at + size] for at in range(0, experts, size)]


def shards(
    mixer_in,
    mixer_gain,
    group_weight,
    group_scale,
    expert_in,
    expert_gain,
    routes,
    route_weight,
    gate_weight,
    up_weight,
    down_weight,
):
    experts, members = lax.axis_size("ep"), lax.axis_size("tp")
    count, width = expert_in.shape
    capacity = max(2, 3 * count * TOP // (2 * experts))
    slots = -(-capacity // 16) * 16
    ep, tp = lax.axis_index("ep"), lax.axis_index("tp")
    mixer_count = mixer_in.shape[0]
    place = jnp.stack([ep, tp, (ep * members + tp) * mixer_count]).astype(jnp.int32)
    peers = list(range(0, members, 2))

    total = experts * members
    halo = lax.ppermute(
        mixer_in[mixer_count - WMAX :], ("ep", "tp"), [(i, i + 1) for i in range(total - 1)]
    )

    made = front(
        place, expert_in, expert_gain[None], routes, route_weight, experts, slots
    )
    chunks, high, low = made[:experts], made[experts], made[experts + 1]

    gate, up, down = gate_weight[0], up_weight[0], down_weight[0]
    gates = [gate, swap(gate, "tp", 1)]
    ups = [up, swap(up, "tp", 1)]
    downs = []
    for peer in peers:
        own = swap(down, "tp", peer)
        downs += [own, swap(own, "tp", 1)]

    order = chunk_groups(experts)
    arrived = {k: swap(chunks[k], "ep", k) for group in order for k in group}

    pooled = pool(place, halo, mixer_in, mixer_gain[None], members)
    pooled = [swap(p, "tp", m) for m, p in enumerate(pooled)]

    returned = [None] * experts
    for group in order:
        rows = [[swap(arrived[k], "tp", peer) for k in group] for peer in peers]
        hidden = hidden_of(rows, gates, ups)
        hidden = [swap(h, "tp", peer) for h, peer in zip(hidden, peers)]
        results = result_of(hidden, downs, len(group), slots)
        for k, result in zip(group, results):
            returned[k] = swap(result, "ep", k)

    mixed = mix(place, pooled, group_weight, group_scale)
    return mixed, combine(high, low, returned)


def solution(mesh):
    in_specs = (
        P(("ep", "tp"), None),
        P(),
        P("tp", None, None),
        P("tp", None),
        P(("ep", "tp"), None),
        P(),
        P("ep", None),
        P("ep", None),
        P("ep", None, "tp"),
        P("ep", None, "tp"),
        P("ep", "tp", None),
    )
    out_specs = (P("ep", "tp"), P(("ep", "tp"), None))
    return jax.shard_map(shards, mesh=mesh, in_specs=in_specs, out_specs=out_specs, check_vma=False)
```
